32 devices in a mesh: dp: 4 (over y, x), kv: 4 (over z), tp: 2 (over core).
Axes of the slice: x: 2, y: 2, z: 4, core: 2. Of those that a mesh axis runs over, the one named last changes fastest.
Arguments:
- tokens: bfloat16 [128, 4096], P('dp', ('kv', 'tp')), may hold values from -11.5 to 11.5, as said below
- gain_mix: float32 [4096], replicated, may hold values from 0.1 to 1.9
- gain_mlp: float32 [4096], replicated, may hold values from 0.1 to 1.9
- decay_rate: float32 [16], replicated, may hold values from 0.01 to 1
- w_query: bfloat16 [4096, 1024], P('kv', 'tp'), may hold values from -0.09375 to 0.09375
- w_key: bfloat16 [4096, 1024], P('kv', 'tp'), may hold values from -0.09375 to 0.09375
- w_value: bfloat16 [4096, 2048], P('kv', 'tp'), may hold values from -0.09375 to 0.09375
- w_gate: bfloat16 [4096, 2048], P('kv', 'tp'), may hold values from -0.09375 to 0.09375
- w_mix: bfloat16 [2048, 4096], P('tp', 'kv'), may hold values from -0.125 to 0.125
- w_up: bfloat16 [4096, 16384], P(None, ('kv', 'tp')), may hold values from -0.09375 to 0.09375
- w_down: bfloat16 [16384, 4096], P(('kv', 'tp')), may hold values from -0.0625 to 0.0625
- state: float32 [128, 16, 64, 128], P(('dp', 'kv'), 'tp'), may hold values from -2 to 2
Outputs:
- result: bfloat16 [128, 4096], P('dp', ('kv', 'tp'))
- new_state: float32 [128, 16, 64, 128], P(('dp', 'kv'), 'tp')
The draws below stay inside these ranges and needn't reach their ends.
Inputs may be any that keep to these rules, and one draw needn't show every extreme that they name: `tokens`: feature scales differ across the features.
All inputs are finite; a program needn't handle non-finite values.
Results may differ from the reference program's by a relative error of at most 0.02.
Values may be sent and summed in bfloat16 or wider, within the bound.
A program may use at most 128 MiB of HBM per device.

```python
import math
import jax
import jax.numpy as jnp
from jax import lax

D = 4096
HEADS = 16
DK = 64
DV = 128
FF = 16384
BATCH = 128
N_TP = 2


def draw_tokens(key, part):
    col_scale = jnp.exp(jnp.linspace(jnp.log(0.35), jnp.log(2.8), D)).astype(jnp.float32)
    normal_part = jnp.clip(jax.random.normal(key, (BATCH, D), jnp.float32), -4.0, 4.0)
    values_out = normal_part * col_scale[None, :]
    return values_out.astype(jnp.bfloat16)


def spiked(array, stream_key, source, target, parts, factor):
    def block_of(dim):
        return (jnp.arange(array.shape[dim]) // (array.shape[dim] // parts)).reshape((-1,) + (1,) * (array.ndim - 1 - dim))

    near = jax.random.permutation(stream_key, parts)[block_of(target)]
    far = (block_of(target) + parts // 2) % parts
    return jnp.where((block_of(source) == near) | (block_of(source) == far), factor * array, array)


def block_scale(rng, shape, shards, least, largest):
    def one(position, parts):
        heights = jax.random.uniform(jax.random.fold_in(jax.random.fold_in(rng, 6), position), (parts,), jnp.float32, least / len(shards), largest / len(shards))
        return jnp.repeat(jnp.exp(heights), shape[position] // parts).reshape((-1,) + (1,) * (len(shape) - position - 1))

    gain = one(*shards[0])
    for cut in shards[1:]:
        gain = gain * one(*cut)
    return gain


def scatter_about(own_key, shape, deviation, bound, pieces=(), kind=jnp.bfloat16):
    loudness = block_scale(own_key, shape, pieces, -0.22, 0.18) if pieces else 1.0
    drawn = jax.random.normal(own_key, shape, jnp.float32) * deviation * loudness
    return jnp.minimum(jnp.maximum(drawn, -bound), bound).astype(kind)


def noise_with(own_key, shape, width, limit, pieces, heavy, dtype=jnp.bfloat16):
    entries = width * jax.random.normal(own_key, shape, jnp.float32)
    if pieces:
        entries = entries * block_scale(own_key, shape, pieces, -0.22, 0.18)
    return jnp.clip(spiked(entries, jax.random.fold_in(own_key, 3), *heavy), -limit, limit).astype(dtype)


def setup_inputs(seed: int = 0) -> dict:
    key_list = jax.random.split(jax.random.key(seed), 13)
    tokens = draw_tokens(jax.random.fold_in(key_list[12], 71), 0)
    gain_mix = jnp.clip(1.0 + 0.18 * jax.random.normal(key_list[1], (D,), jnp.float32), 0.1, 1.9)
    gain_mlp = jnp.clip(1.0 + 0.18 * jax.random.normal(key_list[2], (D,), jnp.float32), 0.1, 1.9)
    decay_rate = jnp.clip(jnp.exp(jax.random.uniform(key_list[3], (HEADS,), jnp.float32, math.log(0.01), math.log(1.0))), 0.01, 1.0)
    w_query = scatter_about(key_list[4], (D, HEADS * DK), D ** -0.5, 0.09375, ((0, 4), (1, 2)))
    w_key = scatter_about(key_list[5], (D, HEADS * DK), D ** -0.5, 0.09375, ((0, 4), (1, 2)))
    w_value = scatter_about(key_list[6], (D, HEADS * DV), D ** -0.5, 0.09375, ((0, 4), (1, 2)))
    w_gate = scatter_about(key_list[7], (D, HEADS * DV), D ** -0.5, 0.09375, ((0, 4), (1, 2)))
    w_mix = scatter_about(key_list[8], (HEADS * DV, D), (HEADS * DV) ** -0.5, 0.125, ((0, 2), (1, 4)))
    w_up = scatter_about(key_list[9], (D, FF), D ** -0.5, 0.09375, ((1, 8),))
    w_down = noise_with(key_list[10], (FF, D), FF ** -0.5, 0.0625, ((0, 8),), (0, 1, 8, 2.0))
    state = scatter_about(key_list[11], (BATCH, HEADS, DK, DV), 0.3, 2.0, ((0, 16), (1, 2)), jnp.float32)
    return {"tokens": tokens, "gain_mix": gain_mix, "gain_mlp": gain_mlp, "decay_rate": decay_rate, "w_query": w_query, "w_key": w_key, "w_value": w_value, "w_gate": w_gate, "w_mix": w_mix, "w_up": w_up, "w_down": w_down, "state": state}


EPS = 1e-06

def reference(tokens, gain_mix, gain_mlp, decay_rate, w_query, w_key, w_value, w_gate, w_mix, w_up, w_down, state):
    batch = tokens.shape[0]
    inputs = tokens.astype(jnp.float32)
    first_scale = lax.rsqrt(lax.optimization_barrier(jnp.mean(inputs * inputs, axis=1, keepdims=True)) + EPS)
    normed = (inputs * first_scale * gain_mix).astype(jnp.bfloat16)
    query = jnp.dot(normed, w_query, preferred_element_type=jnp.float32).astype(jnp.bfloat16)
    keys = jnp.dot(normed, w_key, preferred_element_type=jnp.float32).astype(jnp.bfloat16)
    values = jnp.dot(normed, w_value, preferred_element_type=jnp.float32).astype(jnp.bfloat16)
    gates = jnp.dot(normed, w_gate, preferred_element_type=jnp.float32).astype(jnp.bfloat16)
    query_heads = query.astype(jnp.float32).reshape(batch, HEADS, DK)
    key_heads = keys.astype(jnp.float32).reshape(batch, HEADS, DK) * DK ** (-0.5)
    value_heads = values.astype(jnp.float32).reshape(batch, HEADS, DV)
    gate_heads = gates.astype(jnp.float32).reshape(batch, HEADS, DV)
    decay = jnp.exp(-decay_rate)[None, :, None, None]
    new_state = decay * state + key_heads[:, :, :, None] * value_heads[:, :, None, :]
    read = jnp.einsum('bhd,bhde->bhe', query_heads, new_state, precision=lax.Precision.HIGHEST)
    read = read * lax.rsqrt(lax.optimization_barrier(jnp.mean(read * read, axis=2, keepdims=True)) + EPS)
    heads_out = (jax.nn.silu(gate_heads) * read).reshape(batch, HEADS * DV).astype(jnp.bfloat16)
    group = HEADS * DV // N_TP
    mixed = jnp.zeros((batch, D), jnp.float32)
    for index in range(N_TP):
        product = jnp.dot(heads_out[:, index * group:(index + 1) * group], w_mix[index * group:(index + 1) * group], preferred_element_type=jnp.float32)
        rounded = lax.optimization_barrier(product.astype(jnp.bfloat16))
        mixed = mixed + rounded.astype(jnp.float32)
    resid = (inputs + mixed).astype(jnp.bfloat16)
    resid_f = resid.astype(jnp.float32)
    second_scale = lax.rsqrt(lax.optimization_barrier(jnp.mean(resid_f * resid_f, axis=1, keepdims=True)) + EPS)
    normed_mlp = (resid_f * second_scale * gain_mlp).astype(jnp.bfloat16)
    upper = jnp.dot(normed_mlp, w_up, preferred_element_type=jnp.float32)
    hidden = jnp.square(jax.nn.relu(upper)).astype(jnp.bfloat16)
    down = jnp.dot(hidden, w_down, preferred_element_type=jnp.float32)
    result = (resid_f + down).astype(jnp.bfloat16)
    return (result, new_state)
```

```python
import functools
import jax
import jax.numpy as jnp
from jax import lax
from jax.experimental import pallas as pl
from jax.experimental.pallas import tpu as pltpu
from jax.sharding import PartitionSpec as P

EPS = 1e-06


def per_device(
    tokens,
    gain_mix,
    gain_mlp,
    decay_rate,
    w_query,
    w_key,
    w_value,
    w_gate,
    w_mix,
    w_up,
    w_down,
    state,
):
    seq_count, head_count, key_width, value_width = state.shape
    both_cols = lax.all_gather(tokens, "tp", axis=1, tiled=True)
    col_count = both_cols.shape[1]
    col_start = lax.axis_index("kv") * col_count
    model_width = col_count * lax.axis_size("kv")
    block_f = both_cols.astype(jnp.float32)
    squares = jnp.sum(block_f * block_f, axis=1)
    row_total = lax.psum(squares, "kv")
    first_scale = lax.rsqrt(row_total / model_width + EPS)
    gain_cols = lax.dynamic_slice_in_dim(gain_mix, col_start, col_count)
    normed = (block_f * first_scale[:, None] * gain_cols[None, :]).astype(jnp.bfloat16)
    own_inputs = lax.psum_scatter(
        jnp.concatenate(
            [
                jnp.dot(normed, weight, preferred_element_type=jnp.float32)
                for weight in (w_query, w_key, w_value, w_gate)
            ],
            axis=1,
        ).astype(jnp.bfloat16),
        "kv",
        scatter_dimension=0,
        tiled=True,
    )
    query_end = head_count * key_width
    key_end = 2 * query_end
    value_end = key_end + head_count * value_width
    query_heads = (
        own_inputs[:, :query_end].astype(jnp.float32).reshape(seq_count, head_count, key_width)
    )
    key_heads = (
        own_inputs[:, query_end:key_end]
        .astype(jnp.float32)
        .reshape(seq_count, head_count, key_width)
    )
    key_heads = key_heads * key_width ** (-0.5)
    value_heads = (
        own_inputs[:, key_end:value_end]
        .astype(jnp.float32)
        .reshape(seq_count, head_count, value_width)
    )
    gate_heads = (
        own_inputs[:, value_end:].astype(jnp.float32).reshape(seq_count, head_count, value_width)
    )
    rates = lax.dynamic_slice_in_dim(decay_rate, lax.axis_index("tp") * head_count, head_count)
    decay = jnp.exp(-rates)[None, :, None, None]
    new_state = decay * state + key_heads[:, :, :, None] * value_heads[:, :, None, :]
    read = jnp.einsum("bhd,bhde->bhe", query_heads, new_state, precision=lax.Precision.HIGHEST)
    read = read * lax.rsqrt(jnp.mean(read * read, axis=2, keepdims=True) + EPS)
    heads_out = (
        (jax.nn.silu(gate_heads) * read)
        .reshape(seq_count, head_count * value_width)
        .astype(jnp.bfloat16)
    )
    partial_value = jnp.dot(
        lax.all_gather(heads_out, "kv", axis=0, tiled=True),
        w_mix,
        preferred_element_type=jnp.float32,
    )
    rounded = lax.optimization_barrier(partial_value.astype(jnp.bfloat16)).astype(jnp.float32)
    mixed = lax.psum_scatter(
        rounded.astype(jnp.bfloat16), "tp", scatter_dimension=1, tiled=True
    ).astype(jnp.float32)
    resid_own = (tokens.astype(jnp.float32) + mixed).astype(jnp.bfloat16)
    rows_full = lax.all_gather(resid_own, ("kv", "tp"), axis=1, tiled=True)
    rows_f = rows_full.astype(jnp.float32)
    second_scale = lax.rsqrt(jnp.mean(rows_f * rows_f, axis=1, keepdims=True) + EPS)
    normed_mlp = (rows_f * second_scale * gain_mlp[None, :]).astype(jnp.bfloat16)
    upper = jnp.dot(normed_mlp, w_up, preferred_element_type=jnp.float32)
    hidden = jnp.square(jax.nn.relu(upper)).astype(jnp.bfloat16)
    summed = lax.psum_scatter(
        jnp.dot(hidden, w_down, preferred_element_type=jnp.float32),
        ("kv", "tp"),
        scatter_dimension=1,
        tiled=True,
    )
    own_width = tokens.shape[1]
    residual_cols = lax.dynamic_slice_in_dim(
        rows_f, lax.axis_index(("kv", "tp")) * own_width, own_width, 1
    )
    result = (residual_cols + summed).astype(jnp.bfloat16)
    return (result, new_state)


BF = jnp.bfloat16
F32 = jnp.float32


def layer_kernel(
    n,
    tokens_hbm,
    gain_mix_hbm,
    gain_mlp_hbm,
    rate_ref,
    wq_hbm,
    wk_hbm,
    wv_hbm,
    wg_hbm,
    wm_hbm,
    wu_hbm,
    wd_hbm,
    state_hbm,
    result_hbm,
    new_state_hbm,
    tok,
    tok_other,
    gm,
    gl,
    wq,
    wk,
    wv,
    wg,
    wm,
    wu,
    wd,
    st,
    part_out,
    part_in,
    sq_out,
    sq_in,
    own,
    turned,
    heads,
    mix_out,
    mix_in,
    resid,
    upper,
    pair_out,
    pair_in,
    kept,
    sum_out,
    sum_in,
    res,
    local_sem,
    up_sem,
    down_sem,
    tok_sem,
    part_send,
    part_recv,
    sq_send,
    sq_recv,
    head_send,
    head_recv,
    mix_sem,
    res_send,
    res_recv,
    fwd_send,
    pair_send,
    pair_recv,
    sum_send,
    sum_recv,
):
    kv = lax.axis_index("kv")
    tp = lax.axis_index("tp")
    other = 1 - tp
    me = 2 * kv + tp
    rows, width = tok.shape
    seqs, head_count, dk, dv = st.shape
    model = 2 * n * width
    pair_width = 2 * width
    offsets = sorted(range(1, n), key=lambda o: (min(o, n - o), o))

    def peer(offset):
        return lax.rem(kv + offset, n)

    def send(src, dst, send_sem, recv_sem, k, t):
        copy = pltpu.make_async_remote_copy(
            src_ref=src,
            dst_ref=dst,
            send_sem=send_sem,
            recv_sem=recv_sem,
            device_id={"kv": k, "tp": t},
            device_id_type=pl.DeviceIdType.MESH,
        )
        copy.start()
        return copy

    def landed(ref, sem):
        pltpu.make_async_copy(ref, ref, sem).wait()

    loads = [
        pltpu.make_async_copy(a, b, local_sem.at[i])
        for i, (a, b) in enumerate(
            (
                (tokens_hbm, tok),
                (gain_mix_hbm, gm),
                (wv_hbm, wv),
                (wg_hbm, wg),
                (wq_hbm, wq),
                (wk_hbm, wk),
                (state_hbm, st),
                (wm_hbm, wm),
                (gain_mlp_hbm, gl),
            )
        )
    ]
    for load in loads:
        load.start()
    up_loads = [
        pltpu.make_async_copy(wu_hbm.at[pl.ds(j * width, width), :], wu.at[j], up_sem.at[j])
        for j in range(2 * n)
    ]
    down_loads = [
        pltpu.make_async_copy(wd_hbm.at[:, pl.ds(j * width, width)], wd.at[j], down_sem.at[j])
        for j in range(2 * n)
    ]

    barrier = pltpu.get_barrier_semaphore()
    for offset in range(n):
        for t in (tp, other) if offset else (other,):
            pl.semaphore_signal(
                barrier,
                inc=1,
                device_id={"kv": peer(offset), "tp": t},
                device_id_type=pl.DeviceIdType.MESH,
            )
    pl.semaphore_wait(barrier, 2 * n - 1)

    loads[0].wait()
    tok_copy = send(tok, tok_other, tok_sem.at[0], tok_sem.at[1], kv, other)
    loads[1].wait()
    tok_copy.wait_recv()
    mine = tok[...].astype(F32)
    theirs = tok_other[...].astype(F32)
    first = tp == 0
    left = jnp.where(first, mine, theirs)
    right = jnp.where(first, theirs, mine)
    both = jnp.concatenate([left, right], axis=1)
    squares = jnp.sum(both * both, axis=1, keepdims=True)
    scaled = (both * gm[:, pl.ds(pl.multiple_of(kv * pair_width, 128), pair_width)]).astype(BF)
    squares = jnp.broadcast_to(squares, (rows, 128))
    for k in range(n):
        sq_out[k] = squares[k * seqs : (k + 1) * seqs]
    q_width, v_width = wq.shape[1], wv.shape[1]
    starts = (2 * q_width, 2 * q_width + v_width, 0, q_width)
    for index, weight in enumerate((wv, wg, wq, wk)):
        loads[2 + index].wait()
        product = jnp.dot(scaled, weight[...], preferred_element_type=F32)
        cols = slice(starts[index], starts[index] + weight.shape[1])
        for k in range(n):
            part_out[k, :, cols] = product[k * seqs : (k + 1) * seqs].astype(BF)
    sent = []
    for offset in reversed(offsets):
        k = peer(offset)
        sent.append(send(sq_out.at[k], sq_in.at[kv], sq_send.at[offset], sq_recv.at[kv], k, tp))
        sent.append(
            send(part_out.at[k], part_in.at[kv], part_send.at[offset], part_recv.at[kv], k, tp)
        )
    for load in up_loads + down_loads:
        load.start()
    total = part_out[kv].astype(F32)
    sq_total = sq_out[kv]
    for offset in offsets:
        k = peer(offset)
        landed(sq_in.at[k], sq_recv.at[k])
        landed(part_in.at[k], part_recv.at[k])
        total += part_in[k].astype(F32)
        sq_total += sq_in[k]
    total = total * lax.rsqrt(sq_total / model + EPS)[:, :1]
    own[...] = total
    blank = jnp.zeros((128 - 2 * seqs, q_width), F32)
    turned[...] = jnp.concatenate(
        [total[:, :q_width], total[:, q_width : 2 * q_width] * dk ** (-0.5), blank], axis=0
    ).T
    loads[6].wait()

    def one_head(h, carry):
        cols = turned[pl.ds(pl.multiple_of(h * dk, dk), dk), :]
        value = own[:, pl.ds(pl.multiple_of(2 * q_width + h * dv, 128), dv)]
        gate = own[:, pl.ds(pl.multiple_of(2 * q_width + v_width + h * dv, 128), dv)]
        decay = jnp.exp(jnp.full((1, dv), -rate_ref[tp * head_count + h], F32))
        reads = []
        for b in range(seqs):
            new = decay * st[b, h] + cols[:, seqs + b : seqs + b + 1] * value[b : b + 1]
            st[b, h] = new
            reads.append(jnp.sum(cols[:, b : b + 1] * new, axis=0, keepdims=True))
        read = jnp.concatenate(reads, axis=0)
        read = read * lax.rsqrt(jnp.mean(read * read, axis=1, keepdims=True) + EPS)
        out = gate / (1.0 + jnp.exp(-gate)) * read
        heads[kv, :, pl.ds(pl.multiple_of(h * dv, 128), dv)] = out.astype(BF)
        return carry

    lax.fori_loop(0, head_count, one_head, 0)
    for offset in reversed(offsets):
        sent.append(
            send(heads.at[kv], heads.at[kv], head_send.at[offset], head_recv.at[kv], peer(offset), tp)
        )
    state_copy = pltpu.make_async_copy(st, new_state_hbm, local_sem.at[9])
    state_copy.start()
    loads[7].wait()
    for offset in offsets:
        k = peer(offset)
        landed(heads.at[k], head_recv.at[k])
    gathered = jnp.concatenate([heads[k].astype(F32) for k in range(n)], axis=0).astype(BF)
    mix_out[...] = jnp.dot(
        gathered,
        wm[:, pl.ds(pl.multiple_of(other * width, 128), width)],
        preferred_element_type=F32,
    ).astype(BF)
    mix_copy = send(mix_out, mix_in, mix_sem.at[0], mix_sem.at[1], kv, other)
    own_mix = jnp.dot(
        gathered,
        wm[:, pl.ds(pl.multiple_of(tp * width, 128), width)],
        preferred_element_type=F32,
    ).astype(BF)
    mix_copy.wait_recv()
    resid[me] = (
        tok[...].astype(F32) + (own_mix.astype(F32) + mix_in[...].astype(F32))
    ).astype(BF)
    for offset in reversed(offsets):
        sent.append(
            send(resid.at[me], resid.at[me], res_send.at[offset], res_recv.at[me], peer(offset), tp)
        )
    sent.append(send(resid.at[me], resid.at[me], res_send.at[0], res_recv.at[me], kv, other))
    loads[8].wait()

    def up_step(j, so_far):
        pltpu.make_async_copy(
            wu_hbm.at[pl.ds(0, width), :], wu.at[j], up_sem.at[j]
        ).wait()
        block = resid[j].astype(F32)
        cols = pl.ds(pl.multiple_of(j * width, 128), width)
        product = jnp.dot((block * gl[:, cols]).astype(BF), wu[j], preferred_element_type=F32)
        squares = jnp.sum(block * block, axis=1, keepdims=True)
        if so_far is None:
            upper[...] = product
            return squares
        upper[...] += product
        return so_far + squares

    def direct(offset, so_far):
        j = 2 * peer(offset) + tp
        landed(resid.at[j], res_recv.at[j])
        sent.append(send(resid.at[j], resid.at[j], fwd_send.at[offset], res_recv.at[j], kv, other))
        return up_step(j, so_far)

    def passed(offset, so_far):
        j = 2 * peer(offset) + other
        landed(resid.at[j], res_recv.at[j])
        return up_step(j, so_far)

    row_sq = up_step(me, None)
    row_sq = passed(0, row_sq)
    waiting = []
    for offset in offsets:
        row_sq = direct(offset, row_sq)
        waiting.append(offset)
        if len(waiting) > 1:
            row_sq = passed(waiting.pop(0), row_sq)
    for offset in waiting:
        row_sq = passed(offset, row_sq)
    positive = jnp.maximum(upper[...] * lax.rsqrt(row_sq / model + EPS), 0.0)
    hidden = (positive * positive).astype(BF)

    def down_dot(j):
        pltpu.make_async_copy(
            wd_hbm.at[:, pl.ds(0, width)], wd.at[j], down_sem.at[j]
        ).wait()
        return jnp.dot(hidden, wd[j], preferred_element_type=F32)

    def combine(offset):
        k = peer(offset)
        landed(pair_in.at[k], pair_recv.at[k])
        sum_out[k] = (kept[k] + pair_in[k].astype(F32)).astype(BF)
        sent.append(send(sum_out.at[k], sum_in.at[kv], sum_send.at[offset], sum_recv.at[kv], k, tp))

    pending = None
    for offset in offsets[::-1] + [0]:
        k = peer(offset)
        pair_out[k] = down_dot(2 * k + other).astype(BF)
        sent.append(
            send(pair_out.at[k], pair_in.at[k], pair_send.at[k], pair_recv.at[k], kv, other)
        )
        if pending is not None:
            combine(pending)
        kept[k] = down_dot(2 * k + tp)
        pending = offset
    final = resid[me].astype(F32) + kept[kv]
    landed(pair_in.at[kv], pair_recv.at[kv])
    final += pair_in[kv].astype(F32)
    for offset in offsets:
        k = peer(offset)
        landed(sum_in.at[k], sum_recv.at[k])
        final += sum_in[k].astype(F32)
    res[...] = final.astype(BF)
    out_copy = pltpu.make_async_copy(res, result_hbm, local_sem.at[10])
    out_copy.start()
    tok_copy.wait_send()
    mix_copy.wait_send()
    for copy in sent:
        copy.wait_send()
    state_copy.wait()
    out_copy.wait()


def fused_device(
    n,
    tokens,
    gain_mix,
    gain_mlp,
    decay_rate,
    w_query,
    w_key,
    w_value,
    w_gate,
    w_mix,
    w_up,
    w_down,
    state,
):
    rows, width = tokens.shape
    seqs, head_count, dk, dv = state.shape
    model = gain_mix.shape[0]
    qk_width, v_width = w_query.shape[1], w_value.shape[1]
    all_width = 2 * qk_width + 2 * v_width
    units = w_up.shape[1]
    anywhere = pl.BlockSpec(memory_space=pl.ANY)
    dma = pltpu.SemaphoreType.DMA
    vmem = pltpu.VMEM
    scratch = [
        vmem((rows, width), BF),
        vmem((rows, width), BF),
        vmem((1, model), F32),
        vmem((1, model), F32),
        vmem(w_query.shape, BF),
        vmem(w_key.shape, BF),
        vmem(w_value.shape, BF),
        vmem(w_gate.shape, BF),
        vmem(w_mix.shape, BF),
        vmem((2 * n, width, units), BF),
        vmem((2 * n, units, width), BF),
        vmem(state.shape, F32),
        vmem((n, seqs, all_width), BF),
        vmem((n, seqs, all_width), BF),
        vmem((n, seqs, 128), F32),
        vmem((n, seqs, 128), F32),
        vmem((seqs, all_width), F32),
        vmem((qk_width, 128), F32),
        vmem((n, seqs, v_width), BF),
        vmem((rows, width), BF),
        vmem((rows, width), BF),
        vmem((2 * n, rows, width), BF),
        vmem((rows, units), F32),
        vmem((n, rows, width), BF),
        vmem((n, rows, width), BF),
        vmem((n, rows, width), F32),
        vmem((n, rows, width), BF),
        vmem((n, rows, width), BF),
        vmem((rows, width), BF),
        dma((11,)),
        dma((2 * n,)),
        dma((2 * n,)),
        dma((2,)),
        dma((n,)),
        dma((n,)),
        dma((n,)),
        dma((n,)),
        dma((n,)),
        dma((n,)),
        dma((2,)),
        dma((n,)),
        dma((2 * n,)),
        dma((n,)),
        dma((n,)),
        dma((n,)),
        dma((n,)),
        dma((n,)),
    ]
    return pl.pallas_call(
        functools.partial(layer_kernel, n),
        out_shape=(
            jax.ShapeDtypeStruct(tokens.shape, tokens.dtype),
            jax.ShapeDtypeStruct(state.shape, state.dtype),
        ),
        in_specs=[anywhere] * 3
        + [pl.BlockSpec(memory_space=pltpu.SMEM)]
        + [anywhere] * 8,
        out_specs=(anywhere, anywhere),
        scratch_shapes=scratch,
        compiler_params=pltpu.CompilerParams(
            collective_id=0, has_side_effects=True, vmem_limit_bytes=60 * 1024 * 1024
        ),
        name="retention_layer",
    )(
        tokens,
        gain_mix.reshape(1, model),
        gain_mlp.reshape(1, model),
        decay_rate,
        w_query,
        w_key,
        w_value,
        w_gate,
        w_mix,
        w_up,
        w_down,
        state,
    )


def device_program(n, n_tp, tokens, *rest):
    state = rest[-1]
    rows, width = tokens.shape
    seqs, head_count, dk, dv = state.shape
    w_query, w_up = rest[3], rest[8]
    weight_bytes = 2 * sum(weight.size for weight in rest[3:-1])
    fits = weight_bytes + 4 * state.size <= 48 * 1024 * 1024
    aligned = (
        width % 128 == 0
        and dv % 128 == 0
        and w_query.shape[1] % 128 == 0
        and w_up.shape[1] % 128 == 0
        and dk % 8 == 0
        and seqs % 8 == 0
        and 2 * seqs <= 128
    )
    if n_tp == 2 and fits and aligned:
        return fused_device(n, tokens, *rest)
    return per_device(tokens, *rest)


def solution(mesh):
    placed = (
        P("dp", ("kv", "tp")),
        P(),
        P(),
        P(),
        P("kv", "tp"),
        P("kv", "tp"),
        P("kv", "tp"),
        P("kv", "tp"),
        P("tp", "kv"),
        P(None, ("kv", "tp")),
        P(("kv", "tp"), None),
        P(("dp", "kv"), "tp", None, None),
    )
    return jax.shard_map(
        functools.partial(device_program, mesh.shape["kv"], mesh.shape["tp"]),
        mesh=mesh,
        in_specs=placed,
        out_specs=(P("dp", ("kv", "tp")), P(("dp", "kv"), "tp", None, None)),
        check_vma=False,
    )
```

```python
import functools
import jax
import jax.numpy as jnp
from jax import lax
from jax.experimental import pallas as pl
from jax.experimental.pallas import tpu as pltpu
from jax.sharding import PartitionSpec as P

EPS = 1e-06


def per_device(
    tokens,
    gain_mix,
    gain_mlp,
    decay_rate,
    w_query,
    w_key,
    w_value,
    w_gate,
    w_mix,
    w_up,
    w_down,
    state,
):
    seq_count, head_count, key_width, value_width = state.shape
    both_cols = lax.all_gather(tokens, "tp", axis=1, tiled=True)
    col_count = both_cols.shape[1]
    col_start = lax.axis_index("kv") * col_count
    model_width = col_count * lax.axis_size("kv")
    block_f = both_cols.astype(jnp.float32)
    squares = jnp.sum(block_f * block_f, axis=1)
    row_total = lax.psum(squares, "kv")
    first_scale = lax.rsqrt(row_total / model_width + EPS)
    gain_cols = lax.dynamic_slice_in_dim(gain_mix, col_start, col_count)
    normed = (block_f * first_scale[:, None] * gain_cols[None, :]).astype(jnp.bfloat16)
    own_inputs = lax.psum_scatter(
        jnp.concatenate(
            [
                jnp.dot(normed, weight, preferred_element_type=jnp.float32)
                for weight in (w_query, w_key, w_value, w_gate)
            ],
            axis=1,
        ).astype(jnp.bfloat16),
        "kv",
        scatter_dimension=0,
        tiled=True,
    )
    query_end = head_count * key_width
    key_end = 2 * query_end
    value_end = key_end + head_count * value_width
    query_heads = (
        own_inputs[:, :query_end].astype(jnp.float32).reshape(seq_count, head_count, key_width)
    )
    key_heads = (
        own_inputs[:, query_end:key_end]
        .astype(jnp.float32)
        .reshape(seq_count, head_count, key_width)
    )
    key_heads = key_heads * key_width ** (-0.5)
    value_heads = (
        own_inputs[:, key_end:value_end]
        .astype(jnp.float32)
        .reshape(seq_count, head_count, value_width)
    )
    gate_heads = (
        own_inputs[:, value_end:].astype(jnp.float32).reshape(seq_count, head_count, value_width)
    )
    rates = lax.dynamic_slice_in_dim(decay_rate, lax.axis_index("tp") * head_count, head_count)
    decay = jnp.exp(-rates)[None, :, None, None]
    new_state = decay * state + key_heads[:, :, :, None] * value_heads[:, :, None, :]
    read = jnp.einsum("bhd,bhde->bhe", query_heads, new_state, precision=lax.Precision.HIGHEST)
    read = read * lax.rsqrt(jnp.mean(read * read, axis=2, keepdims=True) + EPS)
    heads_out = (
        (jax.nn.silu(gate_heads) * read)
        .reshape(seq_count, head_count * value_width)
        .astype(jnp.bfloat16)
    )
    partial_value = jnp.dot(
        lax.all_gather(heads_out, "kv", axis=0, tiled=True),
        w_mix,
        preferred_element_type=jnp.float32,
    )
    rounded = lax.optimization_barrier(partial_value.astype(jnp.bfloat16)).astype(jnp.float32)
    mixed = lax.psum_scatter(
        rounded.astype(jnp.bfloat16), "tp", scatter_dimension=1, tiled=True
    ).astype(jnp.float32)
    resid_own = (tokens.astype(jnp.float32) + mixed).astype(jnp.bfloat16)
    rows_full = lax.all_gather(resid_own, ("kv", "tp"), axis=1, tiled=True)
    rows_f = rows_full.astype(jnp.float32)
    second_scale = lax.rsqrt(jnp.mean(rows_f * rows_f, axis=1, keepdims=True) + EPS)
    normed_mlp = (rows_f * second_scale * gain_mlp[None, :]).astype(jnp.bfloat16)
    upper = jnp.dot(normed_mlp, w_up, preferred_element_type=jnp.float32)
    hidden = jnp.square(jax.nn.relu(upper)).astype(jnp.bfloat16)
    summed = lax.psum_scatter(
        jnp.dot(hidden, w_down, preferred_element_type=jnp.float32),
        ("kv", "tp"),
        scatter_dimension=1,
        tiled=True,
    )
    own_width = tokens.shape[1]
    residual_cols = lax.dynamic_slice_in_dim(
        rows_f, lax.axis_index(("kv", "tp")) * own_width, own_width, 1
    )
    result = (residual_cols + summed).astype(jnp.bfloat16)
    return (result, new_state)


BF = jnp.bfloat16
F32 = jnp.float32


def layer_kernel(
    n,
    tokens_hbm,
    gain_mix_hbm,
    gain_mlp_hbm,
    rate_ref,
    wq_hbm,
    wk_hbm,
    wv_hbm,
    wg_hbm,
    wm_hbm,
    wu_hbm,
    wd_hbm,
    state_hbm,
    res,
    st,
    tok,
    tok_other,
    gm,
    gl,
    wq,
    wk,
    wv,
    wg,
    wm,
    wu,
    wd,
    half_done,
    qk_out,
    qk_in,
    v_out,
    v_in,
    g_out,
    g_in,
    sq_out,
    sq_in,
    own_v,
    own_read,
    turned,
    heads,
    mix_out,
    mix_in,
    resid,
    upper,
    pair_out,
    pair_in,
    kept,
    sum_out,
    sum_in,
    local_sem,
    up_sem,
    down_sem,
    tok_sem,
    part_send,
    part_recv,
    sq_send,
    sq_recv,
    head_send,
    head_recv,
    mix_sem,
    res_send,
    res_recv,
    fwd_send,
    pair_send,
    pair_recv,
    sum_send,
    sum_recv,
):
    kv = lax.axis_index("kv")
    tp = lax.axis_index("tp")
    other = 1 - tp
    me = 2 * kv + tp
    rows, width = tok.shape
    seqs, head_count, dk, dv = st.shape
    model = 2 * n * width
    pair_width = 2 * width
    upper_half = kv // (n // 2)

    def far_peer(i):
        after = 1 - (kv - i - 1 + n) // n
        above = 1 - (kv - (n - 1 - i) + n) // n
        from_top = n - 2 - i + above
        return (1 - upper_half) * from_top + upper_half * (i + after)

    far = [far_peer(i) for i in range(n - 1)]
    near = far[::-1]

    def send(src, dst, send_sem, recv_sem, k, t):
        copy = pltpu.make_async_remote_copy(
            src_ref=src,
            dst_ref=dst,
            send_sem=send_sem,
            recv_sem=recv_sem,
            device_id={"kv": k, "tp": t},
            device_id_type=pl.DeviceIdType.MESH,
        )
        copy.start()
        return copy

    def landed(ref, sem):
        pltpu.make_async_copy(ref, ref, sem).wait()

    loads = [
        pltpu.make_async_copy(a, b, local_sem.at[i])
        for i, (a, b) in enumerate(
            (
                (tokens_hbm, tok),
                (gain_mix_hbm, gm),
                (wq_hbm, wq),
                (wk_hbm, wk),
                (wv_hbm, wv),
                (wg_hbm, wg),
                (state_hbm, st),
                (wm_hbm, wm),
                (gain_mlp_hbm, gl),
            )
        )
    ]
    for load in loads:
        load.start()
    up_loads = [
        pltpu.make_async_copy(wu_hbm.at[pl.ds(j * width, width), :], wu.at[j], up_sem.at[j])
        for j in range(2 * n)
    ]
    down_loads = [
        pltpu.make_async_copy(wd_hbm.at[:, pl.ds(j * width, width)], wd.at[j], down_sem.at[j])
        for j in range(2 * n)
    ]

    barrier = pltpu.get_barrier_semaphore()
    for k in far + [kv]:
        for t in (other,) if k is kv else (other, tp):
            pl.semaphore_signal(
                barrier,
                inc=1,
                device_id={"kv": k, "tp": t},
                device_id_type=pl.DeviceIdType.MESH,
            )
    pl.semaphore_wait(barrier, 2 * n - 1)

    loads[0].wait()
    tok_copy = send(tok, tok_other, tok_sem.at[0], tok_sem.at[1], kv, other)
    loads[1].wait()

    def half_of(half, block):
        cols = pl.ds(pl.multiple_of(kv * pair_width + half * width, 128), width)
        values = block[...].astype(F32)
        return (values * gm[:, cols]).astype(BF), jnp.sum(values * values, axis=1, keepdims=True)

    q_width, v_width = wq.shape[1], wv.shape[1]
    k_at, v_at, g_at = q_width, 2 * q_width, 2 * q_width + v_width
    weights = ((wq, 0, loads[2]), (wk, k_at, loads[3]), (wv, v_at, loads[4]), (wg, g_at, loads[5]))
    scaled, own_squares = half_of(tp, tok)
    own_rows = pl.ds(pl.multiple_of(tp * width, 128), width)
    for weight, start, load in weights:
        load.wait()
        product = jnp.dot(scaled, weight[own_rows, :], preferred_element_type=F32)
        half_done[:, start : start + weight.shape[1]] = product
    tok_copy.wait_recv()
    scaled, squares = half_of(other, tok_other)
    squares = jnp.broadcast_to(squares + own_squares, (rows, 128))
    for k in range(n):
        sq_out[k] = squares[k * seqs : (k + 1) * seqs]
    sent = []
    for i, k in enumerate(far):
        sent.append(send(sq_out.at[k], sq_in.at[kv], sq_send.at[i], sq_recv.at[kv], k, tp))
    other_rows = pl.ds(pl.multiple_of(other * width, 128), width)
    parts = ((qk_out, qk_in), (v_out, v_in), (g_out, g_in))

    def finish(weight, start, part, at):
        product = jnp.dot(scaled, weight[other_rows, :], preferred_element_type=F32)
        product += half_done[:, start : start + weight.shape[1]]
        for k in range(n):
            parts[part][0][k, :, at : at + weight.shape[1]] = product[
                k * seqs : (k + 1) * seqs
            ].astype(BF)

    def scatter(part):
        source, target = parts[part]
        for i, k in enumerate(far):
            sent.append(
                send(
                    source.at[k],
                    target.at[kv],
                    part_send.at[part, i],
                    part_recv.at[part, kv],
                    k,
                    tp,
                )
            )

    def collect(part):
        source, target = parts[part]
        total = source[kv].astype(F32)
        for k in near:
            landed(target.at[k], part_recv.at[part, k])
            total += target[k].astype(F32)
        return total * first_scale

    finish(wq, 0, 0, 0)
    finish(wk, k_at, 0, q_width)
    scatter(0)
    finish(wv, v_at, 1, 0)
    scatter(1)
    finish(wg, g_at, 2, 0)
    scatter(2)
    for load in up_loads + down_loads:
        load.start()
    sq_total = sq_out[kv]
    for k in near:
        landed(sq_in.at[k], sq_recv.at[k])
        sq_total += sq_in[k]
    first_scale = lax.rsqrt(sq_total / model + EPS)[:, :1]
    both = collect(0)
    blank = jnp.zeros((128 - 2 * seqs, q_width), F32)
    turned[...] = (
        jnp.concatenate([both[:, :q_width], both[:, q_width:] * dk ** (-0.5), blank], axis=0)
        .T.astype(BF)
        .astype(F32)
    )
    own_v[...] = collect(1)
    loads[6].wait()

    lane = lax.broadcasted_iota(jnp.int32, (dk, 128), 1)
    ones = jnp.ones((128, dv), BF)
    above = jnp.zeros((seqs, dv), F32)
    below = jnp.zeros((128 - 2 * seqs, dv), F32)

    def one_head(h):
        cols = turned[h * dk : (h + 1) * dk, :]
        value = own_v[:, h * dv : (h + 1) * dv]
        value = jnp.concatenate([above, value, below], axis=0).astype(BF)

        def picked(first):
            return jnp.concatenate(
                [jnp.where(lane == first + b, cols, 0.0) for b in range(seqs)], axis=0
            ).astype(BF)

        outer = jnp.dot(picked(seqs), value, preferred_element_type=F32)
        query = jnp.dot(picked(0), ones, preferred_element_type=F32)
        decay = jnp.exp(jnp.full((1, dv), -rate_ref[tp * head_count + h], F32))
        reads = []
        for b in range(seqs):
            new = decay * st[b, h] + outer[b * dk : (b + 1) * dk]
            st[b, h] = new
            reads.append(jnp.sum(query[b * dk : (b + 1) * dk] * new, axis=0, keepdims=True))
        read = jnp.concatenate(reads, axis=0)
        own_read[:, h * dv : (h + 1) * dv] = read * lax.rsqrt(
            jnp.mean(read * read, axis=1, keepdims=True) + EPS
        )

    for h in range(head_count):
        one_head(h)
    gate = collect(2)
    heads[kv] = (gate / (1.0 + jnp.exp(-gate)) * own_read[...]).astype(BF)
    for i, k in enumerate(far):
        sent.append(send(heads.at[kv], heads.at[kv], head_send.at[i], head_recv.at[kv], k, tp))
    loads[7].wait()
    for k in near:
        landed(heads.at[k], head_recv.at[k])
    gathered = jnp.concatenate([heads[k].astype(F32) for k in range(n)], axis=0).astype(BF)
    mix_out[...] = jnp.dot(
        gathered,
        wm[:, pl.ds(pl.multiple_of(other * width, 128), width)],
        preferred_element_type=F32,
    ).astype(BF)
    mix_copy = send(mix_out, mix_in, mix_sem.at[0], mix_sem.at[1], kv, other)
    own_mix = jnp.dot(
        gathered,
        wm[:, pl.ds(pl.multiple_of(tp * width, 128), width)],
        preferred_element_type=F32,
    ).astype(BF)
    mix_copy.wait_recv()
    resid[me] = (
        tok[...].astype(F32) + (own_mix.astype(F32) + mix_in[...].astype(F32))
    ).astype(BF)
    for i, k in enumerate(far):
        sent.append(send(resid.at[me], resid.at[me], res_send.at[i], res_recv.at[me], k, tp))
    sent.append(send(resid.at[me], resid.at[me], res_send.at[n - 1], res_recv.at[me], kv, other))
    loads[8].wait()

    def up_step(j, so_far):
        pltpu.make_async_copy(
            wu_hbm.at[pl.ds(0, width), :], wu.at[j], up_sem.at[j]
        ).wait()
        block = resid[j].astype(F32)
        cols = pl.ds(pl.multiple_of(j * width, 128), width)
        product = jnp.dot((block * gl[:, cols]).astype(BF), wu[j], preferred_element_type=F32)
        squares = jnp.sum(block * block, axis=1, keepdims=True)
        if so_far is None:
            upper[...] = product
            return squares
        upper[...] += product
        return so_far + squares

    def direct(i, so_far):
        j = 2 * near[i] + tp
        landed(resid.at[j], res_recv.at[j])
        sent.append(send(resid.at[j], resid.at[j], fwd_send.at[i], res_recv.at[j], kv, other))
        return up_step(j, so_far)

    def passed(k, so_far):
        j = 2 * k + other
        landed(resid.at[j], res_recv.at[j])
        return up_step(j, so_far)

    row_sq = up_step(me, None)
    row_sq = passed(kv, row_sq)
    for i in range(n - 1):
        row_sq = direct(i, row_sq)
        if i > 0:
            row_sq = passed(near[i - 1], row_sq)
    if n > 1:
        row_sq = passed(near[-1], row_sq)
    positive = jnp.maximum(upper[...] * lax.rsqrt(row_sq / model + EPS), 0.0)
    hidden = (positive * positive).astype(BF)

    def down_dot(j):
        pltpu.make_async_copy(
            wd_hbm.at[:, pl.ds(0, width)], wd.at[j], down_sem.at[j]
        ).wait()
        return jnp.dot(hidden, wd[j], preferred_element_type=F32)

    def for_other(k):
        pair_out[k] = down_dot(2 * k + other).astype(BF)
        sent.append(
            send(pair_out.at[k], pair_in.at[k], pair_send.at[k], pair_recv.at[k], kv, other)
        )

    def combine(i):
        k = far[i]
        kept[k] = down_dot(2 * k + tp)
        landed(pair_in.at[k], pair_recv.at[k])
        sum_out[k] = (kept[k] + pair_in[k].astype(F32)).astype(BF)
        sent.append(send(sum_out.at[k], sum_in.at[kv], sum_send.at[i], sum_recv.at[kv], k, tp))

    for_other(far[0])
    for i in range(n - 1):
        if i < n - 2:
            for_other(far[i + 1])
        combine(i)
    for_other(kv)
    kept[kv] = down_dot(2 * kv + tp)
    final = resid[me].astype(F32) + kept[kv]
    landed(pair_in.at[kv], pair_recv.at[kv])
    final += pair_in[kv].astype(F32)
    for k in near:
        landed(sum_in.at[k], sum_recv.at[k])
        final += sum_in[k].astype(F32)
    res[...] = final.astype(BF)
    tok_copy.wait_send()
    mix_copy.wait_send()
    for copy in sent:
        copy.wait_send()


def write_out(res, st, result_hbm, state_hbm, sems):
    copies = [
        pltpu.make_async_copy(st, state_hbm, sems.at[0]),
        pltpu.make_async_copy(res, result_hbm, sems.at[1]),
    ]
    for copy in copies:
        copy.start()
    for copy in copies:
        copy.wait()


def fused_device(
    n,
    tokens,
    gain_mix,
    gain_mlp,
    decay_rate,
    w_query,
    w_key,
    w_value,
    w_gate,
    w_mix,
    w_up,
    w_down,
    state,
):
    rows, width = tokens.shape
    seqs, head_count, dk, dv = state.shape
    model = gain_mix.shape[0]
    qk_width, v_width = w_query.shape[1], w_value.shape[1]
    all_width = 2 * qk_width + 2 * v_width
    units = w_up.shape[1]
    anywhere = pl.BlockSpec(memory_space=pltpu.HBM)
    inside = pl.BlockSpec(memory_space=pltpu.VMEM)
    dma = pltpu.SemaphoreType.DMA
    vmem = pltpu.VMEM
    scratch = [
        vmem((rows, width), BF),
        vmem((rows, width), BF),
        vmem((1, model), F32),
        vmem((1, model), F32),
        vmem(w_query.shape, BF),
        vmem(w_key.shape, BF),
        vmem(w_value.shape, BF),
        vmem(w_gate.shape, BF),
        vmem(w_mix.shape, BF),
        vmem((2 * n, width, units), BF),
        vmem((2 * n, units, width), BF),
        vmem((rows, all_width), F32),
        vmem((n, seqs, 2 * qk_width), BF),
        vmem((n, seqs, 2 * qk_width), BF),
        vmem((n, seqs, v_width), BF),
        vmem((n, seqs, v_width), BF),
        vmem((n, seqs, v_width), BF),
        vmem((n, seqs, v_width), BF),
        vmem((n, seqs, 128), F32),
        vmem((n, seqs, 128), F32),
        vmem((seqs, v_width), F32),
        vmem((seqs, v_width), F32),
        vmem((qk_width, 128), F32),
        vmem((n, seqs, v_width), BF),
        vmem((rows, width), BF),
        vmem((rows, width), BF),
        vmem((2 * n, rows, width), BF),
        vmem((rows, units), F32),
        vmem((n, rows, width), BF),
        vmem((n, rows, width), BF),
        vmem((n, rows, width), F32),
        vmem((n, rows, width), BF),
        vmem((n, rows, width), BF),
        dma((9,)),
        dma((2 * n,)),
        dma((2 * n,)),
        dma((2,)),
        dma((3, n)),
        dma((3, n)),
        dma((n,)),
        dma((n,)),
        dma((n,)),
        dma((n,)),
        dma((2,)),
        dma((n,)),
        dma((2 * n,)),
        dma((n,)),
        dma((n,)),
        dma((n,)),
        dma((n,)),
        dma((n,)),
    ]
    outs = (
        jax.ShapeDtypeStruct(tokens.shape, tokens.dtype),
        jax.ShapeDtypeStruct(state.shape, state.dtype),
    )
    result, new_state = pl.pallas_call(
        functools.partial(layer_kernel, n),
        out_shape=(vmem(tokens.shape, tokens.dtype), vmem(state.shape, state.dtype)),
        in_specs=[anywhere] * 3
        + [pl.BlockSpec(memory_space=pltpu.SMEM)]
        + [anywhere] * 8,
        out_specs=(inside, inside),
        scratch_shapes=scratch,
        compiler_params=pltpu.CompilerParams(
            collective_id=0, has_side_effects=True, vmem_limit_bytes=64700000
        ),
        name="retention_layer",
    )(
        tokens,
        gain_mix.reshape(1, model),
        gain_mlp.reshape(1, model),
        decay_rate,
        w_query,
        w_key,
        w_value,
        w_gate,
        w_mix,
        w_up,
        w_down,
        state,
    )
    return pl.pallas_call(
        write_out,
        out_shape=outs,
        in_specs=[inside, inside],
        out_specs=(anywhere, anywhere),
        scratch_shapes=[dma((2,))],
        compiler_params=pltpu.CompilerParams(vmem_limit_bytes=4 * 1024 * 1024),
        name="write_out",
    )(result, new_state)


def device_program(n, n_tp, tokens, *rest):
    state = rest[-1]
    rows, width = tokens.shape
    seqs, head_count, dk, dv = state.shape
    w_query, w_up = rest[3], rest[8]
    weight_bytes = 2 * sum(weight.size for weight in rest[3:-1])
    fits = weight_bytes + 4 * state.size <= 48 * 1024 * 1024
    aligned = (
        width % 128 == 0
        and dv % 128 == 0
        and w_query.shape[1] % 128 == 0
        and w_up.shape[1] % 128 == 0
        and dk % 8 == 0
        and seqs % 8 == 0
        and 2 * seqs <= 128
    )
    if n_tp == 2 and n % 2 == 0 and fits and aligned:
        return fused_device(n, tokens, *rest)
    return per_device(tokens, *rest)


def solution(mesh):
    placed = (
        P("dp", ("kv", "tp")),
        P(),
        P(),
        P(),
        P("kv", "tp"),
        P("kv", "tp"),
        P("kv", "tp"),
        P("kv", "tp"),
        P("tp", "kv"),
        P(None, ("kv", "tp")),
        P(("kv", "tp"), None),
        P(("dp", "kv"), "tp", None, None),
    )
    return jax.shard_map(
        functools.partial(device_program, mesh.shape["kv"], mesh.shape["tp"]),
        mesh=mesh,
        in_specs=placed,
        out_specs=(P("dp", ("kv", "tp")), P(("dp", "kv"), "tp", None, None)),
        check_vma=False,
    )
```

```python
import functools
import jax
import jax.numpy as jnp
from jax import lax
from jax.experimental import pallas as pl
from jax.experimental.pallas import tpu as pltpu
from jax.sharding import PartitionSpec as P

EPS = 1e-06


def per_device(
    tokens,
    gain_mix,
    gain_mlp,
    decay_rate,
    w_query,
    w_key,
    w_value,
    w_gate,
    w_mix,
    w_up,
    w_down,
    state,
):
    seq_count, head_count, key_width, value_width = state.shape
    both_cols = lax.all_gather(tokens, "tp", axis=1, tiled=True)
    col_count = both_cols.shape[1]
    col_start = lax.axis_index("kv") * col_count
    model_width = col_count * lax.axis_size("kv")
    block_f = both_cols.astype(jnp.float32)
    squares = jnp.sum(block_f * block_f, axis=1)
    row_total = lax.psum(squares, "kv")
    first_scale = lax.rsqrt(row_total / model_width + EPS)
    gain_cols = lax.dynamic_slice_in_dim(gain_mix, col_start, col_count)
    normed = (block_f * first_scale[:, None] * gain_cols[None, :]).astype(jnp.bfloat16)
    own_inputs = lax.psum_scatter(
        jnp.concatenate(
            [
                jnp.dot(normed, weight, preferred_element_type=jnp.float32)
                for weight in (w_query, w_key, w_value, w_gate)
            ],
            axis=1,
        ).astype(jnp.bfloat16),
        "kv",
        scatter_dimension=0,
        tiled=True,
    )
    query_end = head_count * key_width
    key_end = 2 * query_end
    value_end = key_end + head_count * value_width
    query_heads = (
        own_inputs[:, :query_end].astype(jnp.float32).reshape(seq_count, head_count, key_width)
    )
    key_heads = (
        own_inputs[:, query_end:key_end]
        .astype(jnp.float32)
        .reshape(seq_count, head_count, key_width)
    )
    key_heads = key_heads * key_width ** (-0.5)
    value_heads = (
        own_inputs[:, key_end:value_end]
        .astype(jnp.float32)
        .reshape(seq_count, head_count, value_width)
    )
    gate_heads = (
        own_inputs[:, value_end:].astype(jnp.float32).reshape(seq_count, head_count, value_width)
    )
    rates = lax.dynamic_slice_in_dim(decay_rate, lax.axis_index("tp") * head_count, head_count)
    decay = jnp.exp(-rates)[None, :, None, None]
    new_state = decay * state + key_heads[:, :, :, None] * value_heads[:, :, None, :]
    read = jnp.einsum("bhd,bhde->bhe", query_heads, new_state, precision=lax.Precision.HIGHEST)
    read = read * lax.rsqrt(jnp.mean(read * read, axis=2, keepdims=True) + EPS)
    heads_out = (
        (jax.nn.silu(gate_heads) * read)
        .reshape(seq_count, head_count * value_width)
        .astype(jnp.bfloat16)
    )
    partial_value = jnp.dot(
        lax.all_gather(heads_out, "kv", axis=0, tiled=True),
        w_mix,
        preferred_element_type=jnp.float32,
    )
    rounded = lax.optimization_barrier(partial_value.astype(jnp.bfloat16)).astype(jnp.float32)
    mixed = lax.psum_scatter(
        rounded.astype(jnp.bfloat16), "tp", scatter_dimension=1, tiled=True
    ).astype(jnp.float32)
    resid_own = (tokens.astype(jnp.float32) + mixed).astype(jnp.bfloat16)
    rows_full = lax.all_gather(resid_own, ("kv", "tp"), axis=1, tiled=True)
    rows_f = rows_full.astype(jnp.float32)
    second_scale = lax.rsqrt(jnp.mean(rows_f * rows_f, axis=1, keepdims=True) + EPS)
    normed_mlp = (rows_f * second_scale * gain_mlp[None, :]).astype(jnp.bfloat16)
    upper = jnp.dot(normed_mlp, w_up, preferred_element_type=jnp.float32)
    hidden = jnp.square(jax.nn.relu(upper)).astype(jnp.bfloat16)
    summed = lax.psum_scatter(
        jnp.dot(hidden, w_down, preferred_element_type=jnp.float32),
        ("kv", "tp"),
        scatter_dimension=1,
        tiled=True,
    )
    own_width = tokens.shape[1]
    residual_cols = lax.dynamic_slice_in_dim(
        rows_f, lax.axis_index(("kv", "tp")) * own_width, own_width, 1
    )
    result = (residual_cols + summed).astype(jnp.bfloat16)
    return (result, new_state)


BF = jnp.bfloat16
F32 = jnp.float32


def layer_kernel(
    n,
    tokens_hbm,
    gain_mix_hbm,
    gain_mlp_hbm,
    rate_ref,
    wq_hbm,
    wk_hbm,
    wv_hbm,
    wg_hbm,
    wm_hbm,
    wu_hbm,
    wd_hbm,
    state_hbm,
    res,
    st,
    tok,
    tok_other,
    gm,
    gl,
    wq,
    wk,
    wv,
    wg,
    wm,
    wu,
    wd,
    half_done,
    qk_out,
    qk_in,
    v_out,
    v_in,
    g_out,
    g_in,
    sq_out,
    sq_in,
    own_v,
    own_read,
    turned,
    heads,
    mix_out,
    mix_in,
    resid,
    upper,
    pair_out,
    pair_in,
    kept,
    sum_out,
    sum_in,
    local_sem,
    up_sem,
    down_sem,
    tok_sem,
    part_send,
    part_recv,
    sq_send,
    sq_recv,
    head_send,
    head_recv,
    mix_sem,
    res_send,
    res_recv,
    fwd_send,
    pair_send,
    pair_recv,
    sum_send,
    sum_recv,
):
    kv = lax.axis_index("kv")
    tp = lax.axis_index("tp")
    other = 1 - tp
    me = 2 * kv + tp
    rows, width = tok.shape
    seqs, head_count, dk, dv = st.shape
    model = 2 * n * width
    pair_width = 2 * width
    upper_half = kv // (n // 2)

    def far_peer(i):
        after = 1 - (kv - i - 1 + n) // n
        above = 1 - (kv - (n - 1 - i) + n) // n
        from_top = n - 2 - i + above
        return (1 - upper_half) * from_top + upper_half * (i + after)

    far = [far_peer(i) for i in range(n - 1)]
    near = far[::-1]

    def send(src, dst, send_sem, recv_sem, k, t):
        copy = pltpu.make_async_remote_copy(
            src_ref=src,
            dst_ref=dst,
            send_sem=send_sem,
            recv_sem=recv_sem,
            device_id={"kv": k, "tp": t},
            device_id_type=pl.DeviceIdType.MESH,
        )
        copy.start()
        return copy

    def landed(ref, sem):
        pltpu.make_async_copy(ref, ref, sem).wait()

    loads = [
        pltpu.make_async_copy(a, b, local_sem.at[i])
        for i, (a, b) in enumerate(
            (
                (tokens_hbm, tok),
                (gain_mix_hbm, gm),
                (wq_hbm, wq),
                (wk_hbm, wk),
                (wv_hbm, wv),
                (wg_hbm, wg),
                (state_hbm, st),
                (wm_hbm, wm),
                (gain_mlp_hbm, gl),
            )
        )
    ]
    for load in loads:
        load.start()
    up_loads = [
        pltpu.make_async_copy(wu_hbm.at[pl.ds(j * width, width), :], wu.at[j], up_sem.at[j])
        for j in range(2 * n)
    ]
    down_loads = [
        pltpu.make_async_copy(wd_hbm.at[:, pl.ds(j * width, width)], wd.at[j], down_sem.at[j])
        for j in range(2 * n)
    ]

    barrier = pltpu.get_barrier_semaphore()
    for k in far + [kv]:
        for t in (other,) if k is kv else (other, tp):
            pl.semaphore_signal(
                barrier,
                inc=1,
                device_id={"kv": k, "tp": t},
                device_id_type=pl.DeviceIdType.MESH,
            )
    pl.semaphore_wait(barrier, 2 * n - 1)

    loads[0].wait()
    tok_copy = send(tok, tok_other, tok_sem.at[0], tok_sem.at[1], kv, other)
    loads[1].wait()

    def half_of(half, block):
        cols = pl.ds(pl.multiple_of(kv * pair_width + half * width, 128), width)
        values = block[...].astype(F32)
        return (values * gm[:, cols]).astype(BF), jnp.sum(values * values, axis=1, keepdims=True)

    q_width, v_width = wq.shape[1], wv.shape[1]
    k_at, v_at, g_at = q_width, 2 * q_width, 2 * q_width + v_width
    weights = ((wq, 0, loads[2]), (wk, k_at, loads[3]), (wv, v_at, loads[4]), (wg, g_at, loads[5]))
    scaled, own_squares = half_of(tp, tok)
    own_rows = pl.ds(pl.multiple_of(tp * width, 128), width)
    for weight, start, load in weights:
        load.wait()
        product = jnp.dot(scaled, weight[own_rows, :], preferred_element_type=F32)
        half_done[:, start : start + weight.shape[1]] = product
    tok_copy.wait_recv()
    scaled, squares = half_of(other, tok_other)
    squares = jnp.broadcast_to(squares + own_squares, (rows, 128))
    for k in range(n):
        sq_out[k] = squares[k * seqs : (k + 1) * seqs]
    sent = []
    for i, k in enumerate(far):
        sent.append(send(sq_out.at[k], sq_in.at[kv], sq_send.at[i], sq_recv.at[kv], k, tp))
    other_rows = pl.ds(pl.multiple_of(other * width, 128), width)
    parts = ((qk_out, qk_in), (v_out, v_in), (g_out, g_in))

    def finish(weight, start, part, at):
        product = jnp.dot(scaled, weight[other_rows, :], preferred_element_type=F32)
        product += half_done[:, start : start + weight.shape[1]]
        for k in range(n):
            parts[part][0][k, :, at : at + weight.shape[1]] = product[
                k * seqs : (k + 1) * seqs
            ].astype(BF)

    def scatter(part):
        source, target = parts[part]
        for i, k in enumerate(far):
            sent.append(
                send(
                    source.at[k],
                    target.at[kv],
                    part_send.at[part, i],
                    part_recv.at[part, kv],
                    k,
                    tp,
                )
            )

    def collect(part):
        source, target = parts[part]
        total = source[kv].astype(F32)
        for k in near:
            landed(target.at[k], part_recv.at[part, k])
            total += target[k].astype(F32)
        return total * first_scale

    finish(wq, 0, 0, 0)
    finish(wk, k_at, 0, q_width)
    scatter(0)
    finish(wv, v_at, 1, 0)
    scatter(1)
    finish(wg, g_at, 2, 0)
    scatter(2)
    for load in up_loads + down_loads:
        load.start()
    sq_total = sq_out[kv]
    for k in near:
        landed(sq_in.at[k], sq_recv.at[k])
        sq_total += sq_in[k]
    first_scale = lax.rsqrt(sq_total / model + EPS)[:, :1]
    both = collect(0)
    blank = jnp.zeros((128 - 2 * seqs, q_width), F32)
    turned[...] = (
        jnp.concatenate([both[:, :q_width], both[:, q_width:] * dk ** (-0.5), blank], axis=0)
        .T.astype(BF)
        .astype(F32)
    )
    own_v[...] = collect(1)
    loads[6].wait()

    lane = lax.broadcasted_iota(jnp.int32, (dk, 128), 1)
    ones = jnp.ones((128, dv), BF)
    above = jnp.zeros((seqs, dv), F32)
    below = jnp.zeros((128 - 2 * seqs, dv), F32)

    def one_head(h):
        cols = turned[h * dk : (h + 1) * dk, :]
        value = own_v[:, h * dv : (h + 1) * dv]
        value = jnp.concatenate([above, value, below], axis=0).astype(BF)

        def picked(first):
            return jnp.concatenate(
                [jnp.where(lane == first + b, cols, 0.0) for b in range(seqs)], axis=0
            ).astype(BF)

        outer = jnp.dot(picked(seqs), value, preferred_element_type=F32)
        query = jnp.dot(picked(0), ones, preferred_element_type=F32)
        decay = jnp.exp(jnp.full((1, dv), -rate_ref[tp * head_count + h], F32))
        reads = []
        for b in range(seqs):
            new = decay * st[b, h] + outer[b * dk : (b + 1) * dk]
            st[b, h] = new
            reads.append(jnp.sum(query[b * dk : (b + 1) * dk] * new, axis=0, keepdims=True))
        read = jnp.concatenate(reads, axis=0)
        own_read[:, h * dv : (h + 1) * dv] = read * lax.rsqrt(
            jnp.mean(read * read, axis=1, keepdims=True) + EPS
        )

    for h in range(head_count):
        one_head(h)
    gate = collect(2)
    heads[kv] = (gate / (1.0 + jnp.exp(-gate)) * own_read[...]).astype(BF)
    for i, k in enumerate(far):
        sent.append(send(heads.at[kv], heads.at[kv], head_send.at[i], head_recv.at[kv], k, tp))
    loads[7].wait()
    for k in near:
        landed(heads.at[k], head_recv.at[k])
    gathered = jnp.concatenate([heads[k].astype(F32) for k in range(n)], axis=0).astype(BF)
    mix_out[...] = jnp.dot(
        gathered,
        wm[:, pl.ds(pl.multiple_of(other * width, 128), width)],
        preferred_element_type=F32,
    ).astype(BF)
    mix_copy = send(mix_out, mix_in, mix_sem.at[0], mix_sem.at[1], kv, other)
    own_mix = jnp.dot(
        gathered,
        wm[:, pl.ds(pl.multiple_of(tp * width, 128), width)],
        preferred_element_type=F32,
    ).astype(BF)
    mix_copy.wait_recv()
    resid[me] = (
        tok[...].astype(F32) + (own_mix.astype(F32) + mix_in[...].astype(F32))
    ).astype(BF)
    sent.append(send(resid.at[me], resid.at[me], res_send.at[n - 1], res_recv.at[me], kv, other))
    for i, k in enumerate(near):
        sent.append(send(resid.at[me], resid.at[me], res_send.at[i], res_recv.at[me], k, tp))
    loads[8].wait()

    def up_step(j, so_far):
        pltpu.make_async_copy(
            wu_hbm.at[pl.ds(0, width), :], wu.at[j], up_sem.at[j]
        ).wait()
        block = resid[j].astype(F32)
        cols = pl.ds(pl.multiple_of(j * width, 128), width)
        product = jnp.dot((block * gl[:, cols]).astype(BF), wu[j], preferred_element_type=F32)
        squares = jnp.sum(block * block, axis=1, keepdims=True)
        if so_far is None:
            upper[...] = product
            return squares
        upper[...] += product
        return so_far + squares

    def direct(i, so_far):
        j = 2 * near[i] + tp
        landed(resid.at[j], res_recv.at[j])
        sent.append(send(resid.at[j], resid.at[j], fwd_send.at[i], res_recv.at[j], kv, other))
        return up_step(j, so_far)

    def passed(k, so_far):
        j = 2 * k + other
        landed(resid.at[j], res_recv.at[j])
        return up_step(j, so_far)

    row_sq = up_step(me, None)
    row_sq = passed(kv, row_sq)
    for i in range(n - 1):
        row_sq = direct(i, row_sq)
        if i > 0:
            row_sq = passed(near[i - 1], row_sq)
    if n > 1:
        row_sq = passed(near[-1], row_sq)
    positive = jnp.maximum(upper[...] * lax.rsqrt(row_sq / model + EPS), 0.0)
    hidden = (positive * positive).astype(BF)

    def down_dot(j):
        pltpu.make_async_copy(
            wd_hbm.at[:, pl.ds(0, width)], wd.at[j], down_sem.at[j]
        ).wait()
        return jnp.dot(hidden, wd[j], preferred_element_type=F32)

    def for_other(k):
        pair_out[k] = down_dot(2 * k + other).astype(BF)
        sent.append(
            send(pair_out.at[k], pair_in.at[k], pair_send.at[k], pair_recv.at[k], kv, other)
        )

    def combine(i):
        k = far[i]
        kept[k] = down_dot(2 * k + tp)
        landed(pair_in.at[k], pair_recv.at[k])
        sum_out[k] = (kept[k] + pair_in[k].astype(F32)).astype(BF)
        sent.append(send(sum_out.at[k], sum_in.at[kv], sum_send.at[i], sum_recv.at[kv], k, tp))

    for_other(far[0])
    for i in range(n - 1):
        if i < n - 2:
            for_other(far[i + 1])
        combine(i)
    for_other(kv)
    kept[kv] = down_dot(2 * kv + tp)
    final = resid[me].astype(F32) + kept[kv]
    landed(pair_in.at[kv], pair_recv.at[kv])
    final += pair_in[kv].astype(F32)
    for k in near:
        landed(sum_in.at[k], sum_recv.at[k])
        final += sum_in[k].astype(F32)
    res[...] = final.astype(BF)
    tok_copy.wait_send()
    mix_copy.wait_send()
    for copy in sent:
        copy.wait_send()


def write_out(res, st, result_hbm, state_hbm, sems):
    copies = [
        pltpu.make_async_copy(st, state_hbm, sems.at[0]),
        pltpu.make_async_copy(res, result_hbm, sems.at[1]),
    ]
    for copy in copies:
        copy.start()
    for copy in copies:
        copy.wait()


def fused_device(
    n,
    tokens,
    gain_mix,
    gain_mlp,
    decay_rate,
    w_query,
    w_key,
    w_value,
    w_gate,
    w_mix,
    w_up,
    w_down,
    state,
):
    rows, width = tokens.shape
    seqs, head_count, dk, dv = state.shape
    model = gain_mix.shape[0]
    qk_width, v_width = w_query.shape[1], w_value.shape[1]
    all_width = 2 * qk_width + 2 * v_width
    units = w_up.shape[1]
    anywhere = pl.BlockSpec(memory_space=pltpu.HBM)
    inside = pl.BlockSpec(memory_space=pltpu.VMEM)
    dma = pltpu.SemaphoreType.DMA
    vmem = pltpu.VMEM
    scratch = [
        vmem((rows, width), BF),
        vmem((rows, width), BF),
        vmem((1, model), F32),
        vmem((1, model), F32),
        vmem(w_query.shape, BF),
        vmem(w_key.shape, BF),
        vmem(w_value.shape, BF),
        vmem(w_gate.shape, BF),
        vmem(w_mix.shape, BF),
        vmem((2 * n, width, units), BF),
        vmem((2 * n, units, width), BF),
        vmem((rows, all_width), F32),
        vmem((n, seqs, 2 * qk_width), BF),
        vmem((n, seqs, 2 * qk_width), BF),
        vmem((n, seqs, v_width), BF),
        vmem((n, seqs, v_width), BF),
        vmem((n, seqs, v_width), BF),
        vmem((n, seqs, v_width), BF),
        vmem((n, seqs, 128), F32),
        vmem((n, seqs, 128), F32),
        vmem((seqs, v_width), F32),
        vmem((seqs, v_width), F32),
        vmem((qk_width, 128), F32),
        vmem((n, seqs, v_width), BF),
        vmem((rows, width), BF),
        vmem((rows, width), BF),
        vmem((2 * n, rows, width), BF),
        vmem((rows, units), F32),
        vmem((n, rows, width), BF),
        vmem((n, rows, width), BF),
        vmem((n, rows, width), F32),
        vmem((n, rows, width), BF),
        vmem((n, rows, width), BF),
        dma((9,)),
        dma((2 * n,)),
        dma((2 * n,)),
        dma((2,)),
        dma((3, n)),
        dma((3, n)),
        dma((n,)),
        dma((n,)),
        dma((n,)),
        dma((n,)),
        dma((2,)),
        dma((n,)),
        dma((2 * n,)),
        dma((n,)),
        dma((n,)),
        dma((n,)),
        dma((n,)),
        dma((n,)),
    ]
    outs = (
        jax.ShapeDtypeStruct(tokens.shape, tokens.dtype),
        jax.ShapeDtypeStruct(state.shape, state.dtype),
    )
    result, new_state = pl.pallas_call(
        functools.partial(layer_kernel, n),
        out_shape=(vmem(tokens.shape, tokens.dtype), vmem(state.shape, state.dtype)),
        in_specs=[anywhere] * 3
        + [pl.BlockSpec(memory_space=pltpu.SMEM)]
        + [anywhere] * 8,
        out_specs=(inside, inside),
        scratch_shapes=scratch,
        compiler_params=pltpu.CompilerParams(
            collective_id=0, has_side_effects=True, vmem_limit_bytes=64700000
        ),
        name="retention_layer",
    )(
        tokens,
        gain_mix.reshape(1, model),
        gain_mlp.reshape(1, model),
        decay_rate,
        w_query,
        w_key,
        w_value,
        w_gate,
        w_mix,
        w_up,
        w_down,
        state,
    )
    return pl.pallas_call(
        write_out,
        out_shape=outs,
        in_specs=[inside, inside],
        out_specs=(anywhere, anywhere),
        scratch_shapes=[dma((2,))],
        compiler_params=pltpu.CompilerParams(vmem_limit_bytes=4 * 1024 * 1024),
        name="write_out",
    )(result, new_state)


def device_program(n, n_tp, tokens, *rest):
    state = rest[-1]
    rows, width = tokens.shape
    seqs, head_count, dk, dv = state.shape
    w_query, w_up = rest[3], rest[8]
    weight_bytes = 2 * sum(weight.size for weight in rest[3:-1])
    fits = weight_bytes + 4 * state.size <= 48 * 1024 * 1024
    aligned = (
        width % 128 == 0
        and dv % 128 == 0
        and w_query.shape[1] % 128 == 0
        and w_up.shape[1] % 128 == 0
        and dk % 8 == 0
        and seqs % 8 == 0
        and 2 * seqs <= 128
    )
    if n_tp == 2 and n % 2 == 0 and fits and aligned:
        return fused_device(n, tokens, *rest)
    return per_device(tokens, *rest)


def solution(mesh):
    placed = (
        P("dp", ("kv", "tp")),
        P(),
        P(),
        P(),
        P("kv", "tp"),
        P("kv", "tp"),
        P("kv", "tp"),
        P("kv", "tp"),
        P("tp", "kv"),
        P(None, ("kv", "tp")),
        P(("kv", "tp"), None),
        P(("dp", "kv"), "tp", None, None),
    )
    return jax.shard_map(
        functools.partial(device_program, mesh.shape["kv"], mesh.shape["tp"]),
        mesh=mesh,
        in_specs=placed,
        out_specs=(P("dp", ("kv", "tp")), P(("dp", "kv"), "tp", None, None)),
        check_vma=False,
    )
```
